32 devices in a mesh: ep: 8 (over z, x), tp: 4 (over y, core).
Axes of the slice: x: 2, y: 2, z: 4, core: 2. Of those that a mesh axis runs over, the one named last changes fastest.
Arguments:
- query_rows: bfloat16 [4096, 3072], P('ep', 'tp'), may hold values from -6 to 6
- key_rows: bfloat16 [4096, 1024], P('ep', 'tp'), may hold values from -6 to 6
- value_rows: bfloat16 [4096, 1024], P('ep', 'tp'), may hold values from -6 to 6
- query_gain: float32 [48, 64], P('tp'), may hold values from 0.4 to 48
- key_gain: float32 [16, 64], P('tp'), may hold values from 0.1 to 1.9
- sink_logits: float32 [48], P('tp'), may hold values from 1 to 6
- out_weight: bfloat16 [3072, 2048], P('tp'), may hold values from -0.109375 to 0.109375
- expert_input: bfloat16 [4096, 2048], P(('ep', 'tp')), may hold values from -6 to 6
- expert_gain: float32 [2048], replicated, may hold values from 0.1 to 1.9
- routes: int32 [4096, 2], P(('ep', 'tp')), may hold values from 0 to 31, all different within a row; in each aligned block of 128 rows (0 to 127, 128 to 255, ...) at most 12 rows name the same one
- route_logits: float32 [4096, 2], P(('ep', 'tp')), may hold values from -6 to 6
- gate_weight: bfloat16 [32, 2048, 2048], P('ep', None, 'tp'), may hold values from -0.375 to 0.375
- up_weight: bfloat16 [32, 2048, 2048], P('ep', None, 'tp'), may hold values from -0.375 to 0.375
- down_weight: bfloat16 [32, 2048, 2048], P('ep', 'tp'), may hold values from -0.01953125 to 0.01953125
Outputs:
- attended: bfloat16 [4096, 2048], P(('ep', 'tp'))
- expert_mix: bfloat16 [4096, 2048], P(('ep', 'tp'))
The draws below stay inside these ranges and needn't reach their ends.
Inputs may be any that keep to these rules, and one draw needn't show every extreme that they name: `routes`: each row names 2 different experts; in the rows of one device no expert is named more than 12 times, and in some device one expert is named exactly 12 times.
All inputs are finite; a program needn't handle non-finite values.
Results may differ from the reference program's by a relative error of at most 0.017.
The reference program's roundings to bfloat16 on the way count: a program that leaves them out, or rounds other values in their place, can miss the bound.
Values may be sent and summed in bfloat16 or wider, within the bound.
A program may use at most 128 MiB of HBM per device.

```python
import math
import jax
import jax.numpy as jnp
import numpy as np
from jax import lax

WIDTH = 2048
QHEADS = 48
KVHEADS = 16
HEADDIM = 64
FFN = 2048
EXPERTS = 32
TOPK = 2
WINDOW = 128
TOKENS = 4096
ROWS_DEV = 128
CAP = 12
N_TP = 4


def draw_query_gain(key, part):
    head_key, spread_key = jax.random.split(key)
    head_scale = jnp.exp(jax.random.uniform(head_key, (QHEADS, 1), jnp.float32, math.log(0.7), math.log(3.0)))
    spread = 1.0 + 0.18 * jax.random.uniform(spread_key, (QHEADS, HEADDIM), jnp.float32, -1.0, 1.0)
    return head_scale * spread


def levels(stream_key, dims, pieces, least, high):
    factor_of = 1.0
    for dim, parts in pieces:
        draws = jax.random.uniform(jax.random.fold_in(jax.random.fold_in(stream_key, 6), dim), (parts,), jnp.float32, least / len(pieces), high / len(pieces))
        factor_of = factor_of * jnp.repeat(jnp.exp(draws), dims[dim] // parts).reshape((-1,) + (1,) * (len(dims) - 1 - dim))
    return factor_of


def assign_block(own_key, own, number, rows, number_of, top, bound, lean):
    sequence = jax.random.permutation(own_key, number_of)
    packed, ordinary = load_shares(number_of, rows * top, bound, lean, True), load_shares(number_of, rows * top, bound, lean, False)
    places = jnp.arange(number_of)

    def named(lengths, rotation):
        used = int((lengths > 0).sum())
        fixed = max(1, used // 4)
        passed = fixed + (places - fixed + rotation * (used - fixed)) % max(1, number_of - fixed)
        return jnp.zeros((number_of,), jnp.int32).at[sequence[jnp.where(places < fixed, places, passed)]].set(jnp.asarray(lengths, jnp.int32))

    lengths = jnp.where(number % 4 == 0, named(packed, number // 4), named(ordinary, number - number // 4 - 1))
    mixed = jax.random.permutation(jax.random.fold_in(own, 3), number_of)
    source_of, receiver = mixed[0:number_of // 2 * 2:2], mixed[1:number_of // 2 * 2:2]
    room = jnp.minimum(lengths[source_of] - 1, bound - lengths[receiver]) // 2
    room = jnp.where((source_of == sequence[0]) | (receiver == sequence[0]) | (lengths[receiver] == 0), 0, jnp.maximum(room, 0))
    passed = jax.random.randint(jax.random.fold_in(own, 4), (number_of // 2,), 0, 1 << 20) % (room + 1)
    lengths = lengths.at[source_of].add(-passed).at[receiver].add(passed)
    labels = jnp.searchsorted(jnp.cumsum(lengths), jnp.arange(rows * top), side="right").astype(jnp.int32)
    table = labels.reshape(top, rows).T
    table = table[jax.random.permutation(jax.random.fold_in(own, 1), rows)]
    rotation = jax.random.randint(jax.random.fold_in(own, 2), (rows, 1), 0, top)
    return jnp.take_along_axis(table, (jnp.arange(top)[None, :] + rotation) % top, axis=1)


def load_shares(amount, total, most, skew, full):
    loads = [(1 << 20) // math.isqrt(standing ** skew) + 1 for standing in range(1, amount + 1)]
    largest = most if full else min(most, max(-(-total // amount), total * loads[0] // sum(loads)))
    least = 1 if total - largest >= amount - 1 else 0
    given, spare = [largest] + [least] * (amount - 1), total - largest - least * (amount - 1)
    while spare > 0:
        free = [i for i in range(1, amount) if given[i] < largest] or [i for i in range(1, amount) if given[i] < most]
        whole, remaining = sum([loads[i] for i in free]), spare
        for i in free:
            extra = min(most - given[i], max(1, remaining * loads[i] // whole), spare)
            given[i] = given[i] + extra
            spare = spare - extra
    return np.array(given)


def normal_values(key, shape, scale, reach, pieces=(), kind=jnp.bfloat16):
    array = jax.random.normal(key, shape, jnp.float32) * scale
    if len(pieces) > 0:
        array = levels(key, shape, pieces, -0.22, 0.18) * array
    return jnp.clip(array, min=-reach, max=reach).astype(kind)


def setup_inputs(seed: int = 0) -> dict:
    arg_keys = jax.random.split(jax.random.key(seed), 15)
    query_rows = normal_values(arg_keys[0], (TOKENS, QHEADS * HEADDIM), 1.0, 6.0, ((0, 8), (1, 4)))
    key_rows = normal_values(arg_keys[1], (TOKENS, KVHEADS * HEADDIM), 1.0, 6.0, ((0, 8), (1, 4)))
    value_rows = normal_values(arg_keys[2], (TOKENS, KVHEADS * HEADDIM), 1.0, 6.0, ((0, 8), (1, 4)))
    query_gain = draw_query_gain(jax.random.fold_in(arg_keys[14], 71), 0)
    key_gain = jnp.clip(1.0 + 0.18 * jax.random.normal(arg_keys[4], (KVHEADS, HEADDIM), jnp.float32), 0.1, 1.9)
    sink_logits = jnp.clip(1.0 + 5.0 * jax.random.uniform(arg_keys[5], (QHEADS,), jnp.float32) ** levels(arg_keys[5], (QHEADS,), ((0, 4),), -0.2, 0.2), 1.0, 6.0)
    out_weight = normal_values(arg_keys[6], (QHEADS * HEADDIM, WIDTH), (QHEADS * HEADDIM) ** -0.5, 0.109375, ((0, 4),))
    expert_input = normal_values(arg_keys[7], (TOKENS, WIDTH), 1.0, 6.0, ((0, 32),))
    expert_gain = jnp.clip(1.0 + 0.18 * jax.random.normal(arg_keys[8], (WIDTH,), jnp.float32), 0.1, 1.9)
    routes_keys = jax.random.split(jax.random.fold_in(arg_keys[9], 1), TOKENS // ROWS_DEV)
    routes_turns = jax.random.permutation(jax.random.fold_in(arg_keys[9], 3), TOKENS // ROWS_DEV)
    routes = jax.vmap(lambda own, number: assign_block(jax.random.fold_in(arg_keys[9], 2), own, number, ROWS_DEV, EXPERTS, TOPK, CAP, 1))(routes_keys, routes_turns).reshape((TOKENS, TOPK))
    route_logits = normal_values(arg_keys[10], (TOKENS, TOPK), 1.0, 6.0, ((0, 32),), jnp.float32)
    gate_weight = normal_values(arg_keys[11], (EXPERTS, WIDTH, FFN), (WIDTH // 9) ** -0.5, 0.375, ((0, 8), (2, 4)))
    up_weight = normal_values(arg_keys[12], (EXPERTS, WIDTH, FFN), (WIDTH // 9) ** -0.5, 0.375, ((0, 8), (2, 4)))
    down_weight = normal_values(arg_keys[13], (EXPERTS, FFN, WIDTH), (45 * FFN) ** -0.5, 0.01953125, ((0, 8), (1, 4)))
    return dict(query_rows=query_rows, key_rows=key_rows, value_rows=value_rows, query_gain=query_gain, key_gain=key_gain, sink_logits=sink_logits, out_weight=out_weight, expert_input=expert_input, expert_gain=expert_gain, routes=routes, route_logits=route_logits, gate_weight=gate_weight, up_weight=up_weight, down_weight=down_weight)


EPSILON = 1e-06
CLAMP_LIMIT = 7.0
ACT_SLOPE = 1.702
NEGATIVE = -1e+30

def head_norm(row_data, gain_table):
    head_count, head_size = gain_table.shape
    widened = row_data.astype(jnp.float32).reshape(row_data.shape[0], head_count, head_size)
    scaled = widened * lax.rsqrt(lax.optimization_barrier(jnp.mean(widened * widened, axis=-1, keepdims=True)) + EPSILON)
    return (scaled * gain_table).astype(jnp.bfloat16)

def band(padded, blocks):
    tiled = padded.reshape((blocks + 1, WINDOW) + padded.shape[1:])
    return jnp.concatenate([tiled[:-1], tiled[1:]], axis=1)

def blockwise_product(left, right):
    row_total = left.shape[0]
    inner_width = left.shape[1] // N_TP
    left_parts = jnp.transpose(left.reshape(row_total, N_TP, inner_width), (1, 0, 2))
    right_parts = right.reshape(N_TP, inner_width, right.shape[1])

    def accumulate(running, operands):
        left_part, right_part = operands
        partial_value = jnp.dot(left_part, right_part, preferred_element_type=jnp.float32).astype(jnp.bfloat16)
        partial_value = lax.optimization_barrier(partial_value)
        return (running + partial_value.astype(jnp.float32), None)
    running, unused = lax.scan(accumulate, jnp.zeros((row_total, right.shape[1]), jnp.float32), (left_parts, right_parts))
    return running.astype(jnp.bfloat16)

def attention(query_rows, key_rows, value_rows, query_gain, key_gain, sink_logits):
    seq_rows = query_rows.shape[0]
    blocks = seq_rows // WINDOW
    group_size = QHEADS // KVHEADS
    query_hat = head_norm(query_rows, query_gain).reshape(blocks, WINDOW, KVHEADS, group_size, HEADDIM)
    key_hat = head_norm(key_rows, key_gain)
    value_hat = value_rows.reshape(seq_rows, KVHEADS, HEADDIM)
    leading = jnp.zeros((WINDOW, KVHEADS, HEADDIM), jnp.bfloat16)
    key_band = band(jnp.concatenate([leading, key_hat], axis=0), blocks)
    value_band = band(jnp.concatenate([leading, value_hat], axis=0), blocks)
    query_pos = jnp.arange(WINDOW, dtype=jnp.int32)[:, None]
    key_pos = jnp.arange(2 * WINDOW, dtype=jnp.int32)[None, :]
    distance = query_pos + WINDOW - key_pos
    inside = (distance >= 0) & (distance < WINDOW)
    first_block = (jnp.arange(blocks, dtype=jnp.int32) == 0)[:, None, None]
    allowed = inside[None] & ~(first_block & (key_pos < WINDOW)[None])

    def one_head(operands):
        query_part, key_part, value_part, sink_part = operands
        scores = jnp.einsum('bqgd,bjd->bgqj', query_part.astype(jnp.float32), key_part.astype(jnp.float32), precision=lax.Precision.HIGHEST) * HEADDIM ** (-0.5)
        scores = jnp.where(allowed[:, None], scores, NEGATIVE)
        sink_table = sink_part.reshape(1, group_size, 1, 1)
        highest = jnp.maximum(lax.optimization_barrier(jnp.max(scores, axis=-1, keepdims=True)), sink_table)
        weights = jnp.exp(scores - highest)
        total = lax.optimization_barrier(jnp.sum(weights, axis=-1, keepdims=True)) + jnp.exp(sink_table - highest)
        rounded = lax.optimization_barrier(weights.astype(jnp.bfloat16))
        mixed = jnp.einsum('bgqj,bjd->bgqd', rounded.astype(jnp.float32), value_part.astype(jnp.float32), precision=lax.Precision.HIGHEST)
        return (mixed / total).astype(jnp.bfloat16)
    heads_out = lax.map(one_head, (jnp.transpose(query_hat, (2, 0, 1, 3, 4)), jnp.transpose(key_band, (2, 0, 1, 3)), jnp.transpose(value_band, (2, 0, 1, 3)), sink_logits.reshape(KVHEADS, group_size)))
    return jnp.transpose(heads_out, (1, 3, 0, 2, 4)).reshape(seq_rows, QHEADS * HEADDIM)

def slot_maps(route_block):
    flat_routes = route_block.reshape(-1).astype(jnp.int32)
    expert_hot = (flat_routes[:, None] == jnp.arange(EXPERTS, dtype=jnp.int32)[None, :]).astype(jnp.int32)
    before = jnp.cumsum(expert_hot, axis=0) - expert_hot
    return (flat_routes, lax.optimization_barrier(jnp.sum(before * expert_hot, axis=1)).astype(jnp.int32))

def experts_part(expert_input, expert_gain, routes, route_logits, gate_weight, up_weight, down_weight):
    token_count = expert_input.shape[0]
    block_count = token_count // ROWS_DEV
    widened = expert_input.astype(jnp.float32)
    normed = (widened * lax.rsqrt(lax.optimization_barrier(jnp.mean(widened * widened, axis=-1, keepdims=True)) + EPSILON) * expert_gain).astype(jnp.bfloat16)
    route_weight = jax.nn.softmax(route_logits, axis=-1)
    flat_routes, position = jax.vmap(slot_maps)(routes.reshape(block_count, ROWS_DEV, TOPK))
    row_index = jnp.repeat(jnp.arange(ROWS_DEV, dtype=jnp.int32), TOPK)
    block_index = jnp.arange(block_count, dtype=jnp.int32)[:, None]
    sources = jnp.broadcast_to(row_index[None], flat_routes.shape) + block_index * ROWS_DEV
    table = jnp.full((block_count, EXPERTS, CAP), -1, jnp.int32).at[block_index, flat_routes, position].set(sources)
    tables = jnp.transpose(table, (1, 0, 2)).reshape(EXPERTS, block_count * CAP)

    def one_expert(operands):
        slot_index, gate_part, up_part, down_part = operands
        picked = jnp.where((slot_index >= 0)[:, None], normed[jnp.maximum(slot_index, 0).astype(jnp.int32)], jnp.zeros((), jnp.bfloat16))
        gate_pre = jnp.dot(picked, gate_part, preferred_element_type=jnp.float32)
        up_pre = jnp.dot(picked, up_part, preferred_element_type=jnp.float32)
        clipped = jnp.minimum(gate_pre, CLAMP_LIMIT)
        linear = jnp.clip(up_pre, -CLAMP_LIMIT, CLAMP_LIMIT)
        hidden_units = (clipped * jax.nn.sigmoid(ACT_SLOPE * clipped) * (linear + 1.0)).astype(jnp.bfloat16)
        return blockwise_product(hidden_units, down_part)
    outputs = lax.map(one_expert, (tables, gate_weight, up_weight, down_weight))
    slot_place = (block_index * CAP + position).astype(jnp.int32)
    gathered = outputs[flat_routes, slot_place]
    weighted = gathered.astype(jnp.float32).reshape(block_count, ROWS_DEV, TOPK, WIDTH) * route_weight.reshape(block_count, ROWS_DEV, TOPK, 1)
    return lax.optimization_barrier(jnp.sum(weighted, axis=2)).reshape(token_count, WIDTH).astype(jnp.bfloat16)

def reference(query_rows, key_rows, value_rows, query_gain, key_gain, sink_logits, out_weight, expert_input, expert_gain, routes, route_logits, gate_weight, up_weight, down_weight):
    heads_out = attention(query_rows, key_rows, value_rows, query_gain, key_gain, sink_logits)
    attended = blockwise_product(heads_out, out_weight)
    expert_mix = experts_part(expert_input, expert_gain, routes, route_logits, gate_weight, up_weight, down_weight)
    return (attended, expert_mix)
```

```python
import jax
import jax.numpy as jnp
from jax import lax
from jax.experimental import pallas as pl
from jax.experimental.pallas import tpu as pltpu
from jax.sharding import PartitionSpec as P

EXPERTS = 32
WINDOW = 128


EPSILON = 1e-06
CLAMP_LIMIT = 7.0
ACT_SLOPE = 1.702
NEGATIVE = -1e30


def shifted(value, axis, steps):
    count = lax.axis_size(axis)
    initial, last = (max(0, -steps), min(count, count - steps))
    return lax.ppermute(value, axis, [(source, source + steps) for source in range(initial, last)])


def head_norm(row_data, gain_table):
    head_count, head_size = gain_table.shape
    widened = row_data.astype(jnp.float32).reshape(row_data.shape[0], head_count, head_size)
    scaled = widened * lax.rsqrt(jnp.mean(widened * widened, axis=-1, keepdims=True) + EPSILON)
    return (scaled * gain_table).astype(jnp.bfloat16)


def band(padded, blocks):
    tiled = padded.reshape((blocks + 1, WINDOW) + padded.shape[1:])
    return jnp.concatenate([tiled[:-1], tiled[1:]], axis=1)


def attend(query_rows, key_rows, value_rows, query_gain, key_gain, sink_logits):
    seq_rows = query_rows.shape[0]
    key_heads, head_size = key_gain.shape
    group_size = query_gain.shape[0] // key_heads
    blocks = seq_rows // WINDOW
    query_hat = head_norm(query_rows, query_gain).reshape(
        blocks, WINDOW, key_heads, group_size, head_size
    )
    key_hat = head_norm(key_rows, key_gain)
    value_hat = value_rows.reshape(seq_rows, key_heads, head_size)
    tail_rows = jnp.stack([key_hat[seq_rows - WINDOW :], value_hat[seq_rows - WINDOW :]])
    earlier = shifted(tail_rows, "ep", 1)
    key_band = band(jnp.concatenate([earlier[0], key_hat], axis=0), blocks)
    value_band = band(jnp.concatenate([earlier[1], value_hat], axis=0), blocks)
    query_pos = lax.broadcasted_iota(jnp.int32, (WINDOW, 2 * WINDOW), 0)
    key_pos = lax.broadcasted_iota(jnp.int32, (WINDOW, 2 * WINDOW), 1)
    distance = query_pos + WINDOW - key_pos
    inside = (distance >= 0) & (distance < WINDOW)
    first_block = (lax.broadcasted_iota(jnp.int32, (blocks, 1, 1), 0) == 0) & (
        lax.axis_index("ep") == 0
    )
    allowed = inside[None] & ~(first_block & (key_pos < WINDOW)[None])
    scores = jnp.einsum(
        "bqkgd,bjkd->bkgqj", query_hat, key_band, preferred_element_type=jnp.float32
    ) * head_size ** (-0.5)
    scores = jnp.where(allowed[:, None, None], scores, NEGATIVE)
    sink_table = sink_logits.reshape(1, key_heads, group_size, 1, 1)
    highest = jnp.maximum(jnp.max(scores, axis=-1, keepdims=True), sink_table)
    weights = jnp.exp(scores - highest)
    total = jnp.sum(weights, axis=-1, keepdims=True) + jnp.exp(sink_table - highest)
    mixed = jnp.einsum(
        "bkgqj,bjkd->bkgqd",
        weights.astype(jnp.bfloat16),
        value_band,
        preferred_element_type=jnp.float32,
    )
    mixed = (mixed / total).astype(jnp.bfloat16)
    return jnp.transpose(mixed, (0, 3, 1, 2, 4)).reshape(seq_rows, -1)


def slot_maps(route_block, capacity):
    flat_routes = route_block.reshape(-1)
    expert_hot = (flat_routes[:, None] == lax.broadcasted_iota(jnp.int32, (1, EXPERTS), 1)).astype(
        jnp.int32
    )
    before = jnp.cumsum(expert_hot, axis=0) - expert_hot
    position = jnp.sum(before * expert_hot, axis=1)
    place_hot = (position[:, None] == lax.broadcasted_iota(jnp.int32, (1, capacity), 1)).astype(
        jnp.float32
    )
    row_total, fanout = route_block.shape
    return (
        expert_hot.astype(jnp.float32).reshape(row_total, fanout, EXPERTS),
        place_hot.reshape(row_total, fanout, capacity),
    )


def dispatch_matrix(route_block, capacity):
    expert_hot, place_hot = slot_maps(route_block, capacity)
    return jnp.einsum("rke,rkc->ecr", expert_hot, place_hot).astype(jnp.bfloat16)


def combine_matrix(route_block, route_weight, capacity):
    expert_hot, place_hot = slot_maps(route_block, capacity)
    return jnp.einsum(
        "rke,rkc,rk->rec", expert_hot, place_hot, route_weight, precision=lax.Precision.HIGHEST
    )


def expert_hidden(piece, gate_weight, up_weight):
    gate_pre = jnp.einsum("aecd,edf->aecf", piece, gate_weight, preferred_element_type=jnp.float32)
    up_pre = jnp.einsum("aecd,edf->aecf", piece, up_weight, preferred_element_type=jnp.float32)
    clipped = jnp.minimum(gate_pre, CLAMP_LIMIT)
    linear = jnp.clip(up_pre, -CLAMP_LIMIT, CLAMP_LIMIT)
    return (clipped * jax.nn.sigmoid(ACT_SLOPE * clipped) * (linear + 1.0)).astype(jnp.bfloat16)


MESH = pl.DeviceIdType.MESH


def activation(gate_pre, up_pre):
    clipped = jnp.minimum(gate_pre, CLAMP_LIMIT)
    linear = jnp.clip(up_pre, -CLAMP_LIMIT, CLAMP_LIMIT)
    return (clipped * jax.nn.sigmoid(ACT_SLOPE * clipped) * (linear + 1.0)).astype(jnp.bfloat16)


def expert_kernel(
    dims, slots, perm, unperm, gate_hbm, up_hbm, down_hbm, ret,
    gate_w, up_w, down_w, gath, xbuf, part, dbuf, sums, ybuf,
    wsem, local_sem, zs, zr, ys, yr, ds, dr, rds, rdr, rys, ryr, rzs, rzr,
):
    ep, half, local, cap, rows, width, ffn = dims
    group = 2 * half * cap
    lot = ep // 2
    me = lax.axis_index("ep")
    tp = lax.axis_index("tp")
    hi, core = tp // 2, tp % 2
    other = 1 - core
    partner = hi * 2 + other

    weights = [
        pltpu.make_async_copy(gate_hbm, gate_w, wsem.at[0]),
        pltpu.make_async_copy(up_hbm, up_w, wsem.at[1]),
        pltpu.make_async_copy(down_hbm, down_w, wsem.at[2]),
    ]
    own = pltpu.make_async_copy(slots.at[me], gath.at[me, hi, core], local_sem.at[0])
    own.start()

    barrier = pltpu.get_barrier_semaphore()
    for step in range(1, ep):
        pl.semaphore_signal(barrier, inc=1, device_id=((me + step) % ep, tp), device_id_type=MESH)
    for j in range(1, half):
        pl.semaphore_signal(
            barrier, inc=1, device_id=(me, (hi + j) % half * 2 + core), device_id_type=MESH
        )
    pl.semaphore_signal(barrier, inc=1, device_id=(me, partner), device_id_type=MESH)
    pl.semaphore_wait(barrier, ep - 1 + half - 1 + 1)

    def source(d):
        return (me - d + ep) % ep

    def z_copy(d):
        target = (me + d) % ep
        return pltpu.make_async_remote_copy(
            src_ref=slots.at[target], dst_ref=gath.at[me, hi, core],
            send_sem=zs.at[d], recv_sem=zr.at[d], device_id=(target, tp), device_id_type=MESH,
        )

    def y_copy(d, j):
        s = source(d)
        return pltpu.make_async_remote_copy(
            src_ref=gath.at[s, hi, core], dst_ref=gath.at[s, hi, core],
            send_sem=ys.at[d, j], recv_sem=yr.at[d, j],
            device_id=(me, (hi + j) % half * 2 + core), device_id_type=MESH,
        )

    def d_copy(d, j):
        s = source(d)
        block = (hi - j + half) % half
        return pltpu.make_async_remote_copy(
            src_ref=gath.at[s, block, core], dst_ref=gath.at[s, block, core],
            send_sem=ds.at[d, j], recv_sem=dr.at[d, j],
            device_id=(me, partner), device_id_type=MESH,
        )

    def rd_copy(d, h):
        s = source(d)
        return pltpu.make_async_remote_copy(
            src_ref=part.at[s, h, other], dst_ref=dbuf.at[s, h],
            send_sem=rds.at[d, h], recv_sem=rdr.at[d, h],
            device_id=(me, partner), device_id_type=MESH,
        )

    def ry_copy(d, j):
        s = source(d)
        h = (hi + j) % half
        return pltpu.make_async_remote_copy(
            src_ref=sums.at[s, h], dst_ref=ybuf.at[s, j],
            send_sem=rys.at[d, j], recv_sem=ryr.at[d, j],
            device_id=(me, h * 2 + core), device_id_type=MESH,
        )

    def rz_copy(d):
        s = source(d)
        return pltpu.make_async_remote_copy(
            src_ref=sums.at[s, hi], dst_ref=ret.at[me],
            send_sem=rzs.at[d], recv_sem=rzr.at[d], device_id=(s, tp), device_id_type=MESH,
        )

    def each(first, last, body):
        lax.fori_loop(first, last, lambda i, carry: (body(i), carry)[1], 0)

    each(1, ep, lambda d: z_copy(d).start())
    for copy in weights:
        copy.start()

    def pass_on(d):
        for j in range(1, half):
            y_copy(d, j).start()
        d_copy(d, 0).start()

    def hand_over(d):
        for j in range(1, half):
            y_copy(d, j).wait_recv()
            d_copy(d, j).start()

    def forward(d):
        z_copy(d).wait_recv()
        pass_on(d)
        hand_over(d - 1)

    own.wait()
    pass_on(0)
    each(1, lot, forward)

    tile = min(width, 512)

    def arrange(d, base):
        for j in range(half):
            d_copy(d, j).wait_recv()
        s = source(d)
        at = pl.multiple_of((d - base) * group, 16)
        for col in range(0, width, tile):
            block = gath[s, :, :, :, col : col + tile].reshape(2 * half * rows, tile)
            sorted_rows = jnp.dot(perm[...], block, preferred_element_type=jnp.float32)
            sorted_rows = sorted_rows.astype(jnp.bfloat16)
            for e in range(local):
                xbuf[e, pl.ds(at, group), col : col + tile] = sorted_rows[
                    e * group : (e + 1) * group
                ]

    def expert(e):
        x = xbuf[e]
        hidden = activation(
            jnp.dot(x, gate_w[e], preferred_element_type=jnp.float32),
            jnp.dot(x, up_w[e], preferred_element_type=jnp.float32),
        )
        for col in range(0, width, tile):
            xbuf[e, :, col : col + tile] = jnp.dot(
                hidden, down_w[e, :, col : col + tile], preferred_element_type=jnp.float32
            ).astype(jnp.bfloat16)

    def split(d, base):
        s = source(d)
        at = pl.multiple_of((d - base) * group, 16)
        for col in range(0, width, tile):
            block = jnp.concatenate(
                [xbuf[e, pl.ds(at, group), col : col + tile] for e in range(local)], axis=0
            )
            back = jnp.dot(unperm[...], block, preferred_element_type=jnp.float32)
            part[s, :, :, :, col : col + tile] = back.astype(jnp.bfloat16).reshape(
                half, 2, rows, tile
            )
        for h in range(half):
            rd_copy(d, h).start()

    def join(d):
        s = source(d)
        for h in range(half):
            rd_copy(d, h).wait_recv()
            sums[s, h] = (
                part[s, h, core].astype(jnp.float32) + dbuf[s, h].astype(jnp.float32)
            ).astype(jnp.bfloat16)
        for j in range(1, half):
            ry_copy(d, j).start()

    def finish(d):
        s = source(d)
        total = part[s, hi, core].astype(jnp.float32) + dbuf[s, hi].astype(jnp.float32)
        for j in range(1, half):
            ry_copy(d, j).wait_recv()
            total = total + ybuf[s, j].astype(jnp.float32)
        sums[s, hi] = total.astype(jnp.bfloat16)

    def give_back(d):
        finish(d)
        rz_copy(d).start()

    hand_over(lot - 1)
    each(0, lot, lambda d: arrange(d, 0))
    for copy in weights:
        copy.wait()

    share = lot // local

    def forward_late(d):
        z_copy(d).wait_recv()
        pass_on(d)

        @pl.when(d > lot)
        def _():
            hand_over(d - 1)

    def first_expert(e):
        expert(e)
        for i in range(share):
            forward_late(lot + e * share + i)

    each(0, local, first_expert)
    each(lot + local * share, ep, forward_late)

    def split_join(d, base, first):
        split(d, base)

        @pl.when(d > first)
        def _():
            join(d - 1)

    each(0, lot, lambda d: split_join(d, 0, 0))
    join(lot - 1)
    hand_over(ep - 1)
    each(lot, ep, lambda d: arrange(d, lot))

    finish(0)
    mine = pltpu.make_async_copy(sums.at[me, hi], ret.at[me], local_sem.at[1])
    mine.start()

    def give_early(d):
        @pl.when(d > 0)
        def _():
            give_back(d)

    def second_expert(e):
        expert(e)
        for i in range(share):
            give_early(e * share + i)

    each(0, local, second_expert)
    each(local * share, lot, give_early)
    each(lot, ep, lambda d: split_join(d, lot, lot))
    join(ep - 1)
    each(lot, ep, give_back)
    mine.wait()

    def drain(d):
        for j in range(1, half):
            y_copy(d, j).wait_send()
            ry_copy(d, j).wait_send()
        for j in range(half):
            d_copy(d, j).wait_send()
            rd_copy(d, j).wait_send()

    def drain_far(d):
        z_copy(d).wait_send()
        rz_copy(d).wait()

    each(0, ep, drain)
    each(1, ep, drain_far)


def run_experts(slots, dims, gate_weight, up_weight, down_weight):
    ep, half, local, cap, rows, width, ffn = dims
    tps = 2 * half
    wide = tps * rows
    order = jnp.arange(local * tps * cap)
    e, t, c = order // (tps * cap), order // cap % tps, order % cap
    perm = (t * rows + e * cap + c)[:, None] == jnp.arange(wide)[None, :]
    perm = perm.astype(jnp.bfloat16)
    dma = pltpu.SemaphoreType.DMA
    bf = jnp.bfloat16
    vm = pl.BlockSpec(memory_space=pltpu.VMEM)
    anys = pl.BlockSpec(memory_space=pl.ANY)
    copies = ep * tps * local * cap
    return pl.pallas_call(
        lambda *refs: expert_kernel(dims, *refs),
        name="expert_exchange",
        out_shape=jax.ShapeDtypeStruct((ep, rows, width), bf),
        in_specs=[vm, vm, vm, anys, anys, anys],
        out_specs=vm,
        scratch_shapes=[
            pltpu.VMEM((local, width, ffn), bf),
            pltpu.VMEM((local, width, ffn), bf),
            pltpu.VMEM((local, ffn, width), bf),
            pltpu.VMEM((ep, half, 2, rows, width), bf),
            pltpu.VMEM((local, ep // 2 * tps * cap, width), bf),
            pltpu.VMEM((ep, half, 2, rows, width), bf),
            pltpu.VMEM((ep, half, rows, width), bf),
            pltpu.VMEM((ep, half, rows, width), bf),
            pltpu.VMEM((ep, half, rows, width), bf),
            dma((3,)),
            dma((2,)),
            dma((ep,)), dma((ep,)),
            dma((ep, half)), dma((ep, half)),
            dma((ep, half)), dma((ep, half)),
            dma((ep, half)), dma((ep, half)),
            dma((ep, half)), dma((ep, half)),
            dma((ep,)), dma((ep,)),
        ],
        compiler_params=pltpu.CompilerParams(
            collective_id=0, has_side_effects=True, vmem_limit_bytes=67043328
        ),
        cost_estimate=pl.CostEstimate(
            flops=6 * copies * width * ffn, bytes_accessed=120000000, transcendentals=0
        ),
    )(slots, perm, perm.T, gate_weight, up_weight, down_weight)


def fits(dims):
    ep, half, local, cap, rows, width, ffn = dims
    if half < 1 or ep % 2 or rows % 16 or (2 * half * cap) % 16:
        return False
    held = 3 * local * width * ffn + ep * half * rows * width * 7
    held += ep * half * local * cap * width + 2 * ep * rows * width
    return 2 * held < 60 * 1024 * 1024


def slot_of(routes, cap):
    flat = routes.reshape(-1)
    hot = flat[:, None] == lax.broadcasted_iota(jnp.int32, (1, EXPERTS), 1)
    count = flat.shape[0]
    earlier = lax.broadcasted_iota(jnp.int32, (count, count), 0) > lax.broadcasted_iota(
        jnp.int32, (count, count), 1
    )
    before = jnp.dot(
        earlier.astype(jnp.bfloat16), hot.astype(jnp.bfloat16), preferred_element_type=jnp.float32
    )
    position = jnp.sum(jnp.where(hot, before, 0.0), axis=1).astype(jnp.int32)
    return (flat * cap + position).reshape(routes.shape)


def on_device(
    query_rows,
    key_rows,
    value_rows,
    query_gain,
    key_gain,
    sink_logits,
    out_weight,
    expert_input,
    expert_gain,
    routes,
    route_logits,
    gate_weight,
    up_weight,
    down_weight,
):
    heads_out = attend(query_rows, key_rows, value_rows, query_gain, key_gain, sink_logits)
    projected = jnp.dot(heads_out, out_weight, preferred_element_type=jnp.float32).astype(
        jnp.bfloat16
    )
    own_rows = expert_input.shape[0]
    fanout = routes.shape[1]
    capacity = (3 * own_rows * fanout + 2 * EXPERTS - 1) // (2 * EXPERTS)
    ep_size = lax.axis_size("ep")
    tp_size = lax.axis_size("tp")
    local_experts = gate_weight.shape[0]
    widened = expert_input.astype(jnp.float32)
    normed = (
        widened
        * lax.rsqrt(jnp.mean(widened * widened, axis=-1, keepdims=True) + EPSILON)
        * expert_gain
    ).astype(jnp.bfloat16)
    route_weight = jax.nn.softmax(route_logits, axis=-1)
    dims = (
        ep_size, tp_size // 2, local_experts, capacity, local_experts * capacity,
        expert_input.shape[1], gate_weight.shape[2],
    )
    if fits(dims):
        slot = slot_of(routes, capacity)
        places = lax.broadcasted_iota(jnp.int32, (1, EXPERTS * capacity), 1)
        sender = jnp.zeros((own_rows, EXPERTS * capacity), jnp.bool_)
        combine = jnp.zeros((own_rows, EXPERTS * capacity), jnp.float32)
        for k in range(fanout):
            taken = slot[:, k : k + 1] == places
            sender = sender | taken
            combine = combine + jnp.where(taken, route_weight[:, k : k + 1], 0.0)
        slot_rows = lax.dot_general(
            sender.astype(jnp.bfloat16), normed, (((0,), (0,)), ((), ())),
            preferred_element_type=jnp.float32,
        ).astype(jnp.bfloat16)
        slot_rows, projected = lax.optimization_barrier((slot_rows, projected))
        attended = lax.psum_scatter(projected, "tp", scatter_dimension=0, tiled=True)
        returned = run_experts(
            slot_rows.reshape(ep_size, local_experts * capacity, -1), dims,
            gate_weight, up_weight, down_weight,
        ).reshape(EXPERTS * capacity, -1)
        expert_mix = jnp.dot(
            combine, returned.astype(jnp.float32), precision=lax.Precision.HIGHEST
        ).astype(jnp.bfloat16)
    else:
        attended = lax.psum_scatter(projected, "tp", scatter_dimension=0, tiled=True)
        combine = combine_matrix(routes, route_weight, capacity)
        sender = dispatch_matrix(routes, capacity)
        slot_rows = jnp.einsum(
            "ecr,rd->ecd", sender, normed, preferred_element_type=jnp.float32
        ).astype(jnp.bfloat16)
        slot_rows = slot_rows.reshape(ep_size, local_experts, capacity, -1)
        arrived = lax.all_to_all(slot_rows, "ep", split_axis=0, concat_axis=0, tiled=True)
        hidden_units = expert_hidden(
            lax.all_gather(arrived, "tp", axis=0, tiled=True), gate_weight, up_weight
        )
        partial_value = jnp.einsum(
            "aecf,efd->aecd", hidden_units, down_weight, preferred_element_type=jnp.float32
        ).astype(jnp.bfloat16)
        partial_value = partial_value.reshape(tp_size, ep_size * local_experts * capacity, -1)
        pieces = lax.all_to_all(partial_value, "tp", split_axis=0, concat_axis=0, tiled=True)
        summed = jnp.sum(pieces, axis=0, dtype=jnp.float32).astype(jnp.bfloat16)
        summed = summed.reshape(ep_size, local_experts * capacity, -1)
        returned = lax.all_to_all(summed, "ep", split_axis=0, concat_axis=0, tiled=True).reshape(
            EXPERTS, capacity, -1
        )
        expert_mix = jnp.einsum(
            "rec,ecd->rd", combine, returned.astype(jnp.float32), precision=lax.Precision.HIGHEST
        ).astype(jnp.bfloat16)
    return (attended, expert_mix)


def solution(mesh):
    placed = (
        P("ep", "tp"),
        P("ep", "tp"),
        P("ep", "tp"),
        P("tp", None),
        P("tp", None),
        P("tp"),
        P("tp", None),
        P(("ep", "tp"), None),
        P(),
        P(("ep", "tp"), None),
        P(("ep", "tp"), None),
        P("ep", None, "tp"),
        P("ep", None, "tp"),
        P("ep", "tp", None),
    )
    return jax.shard_map(
        on_device,
        mesh=mesh,
        in_specs=placed,
        out_specs=(P(("ep", "tp"), None), P(("ep", "tp"), None)),
        check_vma=False,
    )
```
